32 devices in a mesh: ep: 8 (over z, core), tp: 4 (over y, x).
Axes of the slice: x: 2, y: 2, z: 4, core: 2. Of those that a mesh axis runs over, the one named last changes fastest.
Arguments:
- hidden: bfloat16 [96, 2048], P('ep'), may hold values from -6 to 6
- pre_gain: bfloat16 [2048], replicated, may hold values from 0.099609375 to 1.8984375
- query_weight: bfloat16 [2048, 1024], P('ep', 'tp'), may hold values from -0.125 to 0.125
- key_cache: bfloat16 [96, 1024, 1024], P('ep', 'tp'), may hold values from -6 to 6
- value_cache: bfloat16 [96, 1024, 1024], P('ep', 'tp'), may hold values from -6 to 6
- lengths: int32 [96], P('ep'), may hold values from 128 to 1024
- stick_bias: float32 [16], P('tp'), may hold values from -8.5 to -3
- out_weight: bfloat16 [1024, 2048], P('tp', 'ep'), may hold values from -0.1875 to 0.1875
- post_gain: bfloat16 [2048], replicated, may hold values from 0.099609375 to 1.8984375
- ffn_gain: bfloat16 [2048], replicated, may hold values from 0.099609375 to 1.8984375
- expert_ids: int32 [96, 2], P('ep'), may hold values from 0 to 7, as said below
- route_logits: float32 [96, 2], P('ep'), may hold values from -6 to 6
- gate_experts: bfloat16 [8, 2048, 2048], P('ep', None, 'tp'), may hold values from -0.125 to 0.125
- up_experts: bfloat16 [8, 2048, 2048], P('ep', None, 'tp'), may hold values from -0.125 to 0.125
- down_experts: bfloat16 [8, 2048, 2048], P('ep', 'tp'), may hold values from -2 to 2
- out_gain: bfloat16 [2048], P('tp'), may hold values from 0.099609375 to 1.8984375
Outputs:
- result: bfloat16 [96, 2048], P('ep', 'tp')
The draws below stay inside these ranges and needn't reach their ends.
Inputs may be any that keep to these rules, and one draw needn't show every extreme that they name: `expert_ids`: each row names 2 different experts of one group of 4 consecutive experts. Among the rows of one device (aligned blocks of 12 rows) no expert is named more than 6 times, and one expert is named exactly 6 times in every block.
All inputs are finite; a program needn't handle non-finite values.
Results may differ from the reference program's by a relative error of at most 0.014.
Values may be sent and summed in bfloat16 or wider, within the bound.
No kernel may reach another device: no remote copies, remote signals or barrier semaphores. Data moves between devices by JAX's collectives and lax.ppermute only.
A program may use at most 64 MiB of HBM per device.

```python
import jax
import jax.numpy as jnp
from jax import lax

D = 2048
HEADS = 16
HEAD = 64
FF = 2048
EXPERTS = 8
EXP_GROUP = 4
TOPK = 2
CACHE = 1024
SEQ_DEV = 12
TOKENS = 96
CAP = 6
N_EP = 8


def draw_expert_ids(key, part):
    groups = EXPERTS // EXP_GROUP
    blocks = TOKENS // SEQ_DEV
    slot_count = groups * CAP
    subkeys = jax.random.split(jax.random.fold_in(key, 11), 6)
    full_group = jax.random.randint(subkeys[0], (), 0, groups)
    full_first = jax.random.randint(subkeys[1], (), 0, EXP_GROUP)
    slot_group = jnp.arange(slot_count, dtype=jnp.int32) // CAP
    scores = jax.random.randint(subkeys[2], (blocks, slot_count), 0, 1 << 20) * slot_count + jnp.arange(slot_count, dtype=jnp.int32)[None, :]
    scores = jnp.where(slot_group[None, :] == full_group, scores - (1 << 26), scores)
    ranking = jnp.argsort(scores, axis=1)[:, :SEQ_DEV]
    chosen = slot_group[ranking]
    shuffle_scores = jax.random.randint(subkeys[3], (blocks, SEQ_DEV), 0, 1 << 20) * SEQ_DEV + jnp.arange(SEQ_DEV, dtype=jnp.int32)[None, :]
    shuffle = jnp.argsort(shuffle_scores, axis=1)
    group_of = jnp.take_along_axis(chosen, shuffle, axis=1)
    first_pick = jax.random.randint(subkeys[4], (blocks, SEQ_DEV), 0, EXP_GROUP)
    first_pick = jnp.where(group_of == full_group, full_first, first_pick)
    offset = jax.random.randint(subkeys[5], (blocks, SEQ_DEV), 1, EXP_GROUP)
    second = (first_pick + offset) % EXP_GROUP
    chosen_ids = jnp.stack([first_pick, second], axis=2) + group_of[:, :, None] * EXP_GROUP
    return chosen_ids.reshape(TOKENS, TOPK).astype(jnp.int32)


def draw_down_experts(key, part):
    base = jax.random.normal(jax.random.fold_in(key, 23), (EXPERTS, FF, D), jnp.float32) * FF ** (-0.5)
    column = jnp.arange(D, dtype=jnp.float32) / D
    column_scale = jnp.exp(jnp.log(10.0) * column) * 0.3
    values = jnp.clip(base * column_scale[None, None, :], -2.0, 2.0)
    return values.astype(jnp.bfloat16)


def place_ends(array, rng, least, high):
    extent = array.shape
    index_at = [jax.random.randint(jax.random.fold_in(rng, axis), (), 0, extent[axis]) for axis in range(len(extent))]
    array = array.at[tuple(index_at)].set(least)
    longest = extent.index(max(extent))
    index_at[longest] = (index_at[longest] + 1) % extent[longest]
    return array.at[tuple(index_at)].set(high)


def steps_of(stream_key, shape, shards, smallest, top_value):
    gain, own = 1.0, jax.random.fold_in(stream_key, 6)
    for axis_at, parts in shards:
        heights = jnp.exp(jax.random.uniform(jax.random.fold_in(own, axis_at), (parts,), jnp.float32, smallest / len(shards), top_value / len(shards)))
        gain = gain * jnp.repeat(heights, shape[axis_at] // parts).reshape([-1 if axis == axis_at else 1 for axis in range(len(shape))])
    return gain


def normal_values(stream_key, shape, deviation, bound, cuts=(), kind=jnp.bfloat16):
    values = jax.random.normal(stream_key, shape, jnp.float32) * deviation
    if len(cuts) > 0:
        values = steps_of(stream_key, shape, cuts, -0.22, 0.18) * values
    return jnp.clip(values, min=-bound, max=bound).astype(kind)


def setup_inputs(seed: int = 0) -> dict:
    splits = jax.random.split(jax.random.key(seed), 17)
    hidden = normal_values(splits[0], (TOKENS, D), 1.0, 6.0, ((0, 8),))
    pre_gain = jnp.clip(1.0 + 0.18 * jax.random.normal(splits[1], (D,), jnp.float32), 0.099609375, 1.8984375).astype(jnp.bfloat16)
    query_weight = normal_values(splits[2], (D, HEADS * HEAD), D ** -0.5, 0.125, ((0, 8), (1, 4)))
    key_cache = normal_values(splits[3], (TOKENS, HEADS * HEAD, CACHE), 1.0, 6.0, ((0, 8), (1, 4)))
    value_cache = normal_values(splits[4], (TOKENS, HEADS * HEAD, CACHE), 1.0, 6.0, ((0, 8), (1, 4)))
    lengths = place_ends(jax.random.randint(splits[5], (TOKENS,), CACHE // 8, CACHE + 1), jax.random.fold_in(splits[5], 1), CACHE // 8, CACHE).astype(jnp.int32)
    stick_bias = jnp.clip(-8.5 + 5.5 * jax.random.uniform(splits[6], (HEADS,), jnp.float32) ** steps_of(splits[6], (HEADS,), ((0, 4),), -0.2, 0.2), -8.5, -3.0)
    out_weight = normal_values(splits[7], (HEADS * HEAD, D), (HEADS * HEAD) ** -0.5, 0.1875, ((0, 4), (1, 8)))
    post_gain = jnp.clip(1.0 + 0.18 * jax.random.normal(splits[8], (D,), jnp.float32), 0.099609375, 1.8984375).astype(jnp.bfloat16)
    ffn_gain = jnp.clip(1.0 + 0.18 * jax.random.normal(splits[9], (D,), jnp.float32), 0.099609375, 1.8984375).astype(jnp.bfloat16)
    expert_ids = draw_expert_ids(jax.random.fold_in(splits[16], 71), 0)
    route_logits = normal_values(splits[11], (TOKENS, TOPK), 1.5, 6.0, ((0, 8),), jnp.float32)
    gate_experts = normal_values(splits[12], (EXPERTS, D, FF), D ** -0.5, 0.125, ((0, 8), (2, 4)))
    up_experts = normal_values(splits[13], (EXPERTS, D, FF), D ** -0.5, 0.125, ((0, 8), (2, 4)))
    down_experts = draw_down_experts(jax.random.fold_in(splits[16], 71), 0)
    out_gain = jnp.clip(1.0 + 0.18 * jax.random.normal(splits[15], (D,), jnp.float32), 0.099609375, 1.8984375).astype(jnp.bfloat16)
    return {"hidden": hidden, "pre_gain": pre_gain, "query_weight": query_weight, "key_cache": key_cache, "value_cache": value_cache, "lengths": lengths, "stick_bias": stick_bias, "out_weight": out_weight, "post_gain": post_gain, "ffn_gain": ffn_gain, "expert_ids": expert_ids, "route_logits": route_logits, "gate_experts": gate_experts, "up_experts": up_experts, "down_experts": down_experts, "out_gain": out_gain}


epsilon = 1e-06

def inverse_rms(squares, features):
    return lax.rsqrt(squares / features + epsilon)

def stick_read(queries, key_blocks, value_blocks, lengths, head_bias):
    sequences, heads, head_size = queries.shape
    positions = key_blocks.shape[3]
    scores = jnp.einsum('she,shec->shc', queries.astype(jnp.float32), key_blocks.astype(jnp.float32))
    scores = scores * head_size ** (-0.5) + head_bias[None, :, None]
    places = lax.broadcasted_iota(jnp.int32, (sequences, heads, positions), 2)
    inside = places < lengths[:, None, None]
    log_fail = jnp.where(inside, jax.nn.log_sigmoid(-scores), 0.0)
    after_sum = lax.cumsum(log_fail, axis=2, reverse=True) - log_fail
    weight = jnp.where(inside, jnp.exp(jax.nn.log_sigmoid(scores) + after_sum), 0.0).astype(jnp.bfloat16)
    weight = lax.optimization_barrier(weight).astype(jnp.float32)
    mixed_heads = jnp.einsum('shc,shec->she', weight, value_blocks.astype(jnp.float32))
    return mixed_heads.astype(jnp.bfloat16)

def reference(hidden, pre_gain, query_weight, key_cache, value_cache, lengths, stick_bias, out_weight, post_gain, ffn_gain, expert_ids, route_logits, gate_experts, up_experts, down_experts, out_gain):
    hidden_wide = hidden.astype(jnp.float32)
    normed = (hidden_wide * inverse_rms(lax.optimization_barrier(jnp.sum(hidden_wide * hidden_wide, axis=1, keepdims=True)), D) * pre_gain.astype(jnp.float32)).astype(jnp.bfloat16)
    queries = jnp.dot(normed, query_weight, preferred_element_type=jnp.float32).astype(jnp.bfloat16)
    queries = queries.reshape(TOKENS, HEADS, HEAD)
    key_blocks = key_cache.reshape(TOKENS, HEADS, HEAD, CACHE)
    value_blocks = value_cache.reshape(TOKENS, HEADS, HEAD, CACHE)

    def one_head(head_index):
        query_head = lax.dynamic_slice_in_dim(queries, head_index, 1, 1)
        key_head = lax.dynamic_slice_in_dim(key_blocks, head_index, 1, 1)
        value_head = lax.dynamic_slice_in_dim(value_blocks, head_index, 1, 1)
        bias_head = lax.dynamic_slice_in_dim(stick_bias, head_index, 1, 0)
        return stick_read(query_head, key_head, value_head, lengths, bias_head)[:, 0, :]
    mixed_heads = lax.map(one_head, jnp.arange(HEADS, dtype=jnp.int32))
    mixed_heads = jnp.transpose(mixed_heads, (1, 0, 2)).reshape(TOKENS, HEADS * HEAD)
    attended = jnp.dot(mixed_heads, out_weight, preferred_element_type=jnp.float32).astype(jnp.bfloat16)
    attended = lax.optimization_barrier(attended).astype(jnp.float32)
    residual = (hidden_wide + attended * inverse_rms(lax.optimization_barrier(jnp.sum(attended * attended, axis=1, keepdims=True)), D) * post_gain.astype(jnp.float32)).astype(jnp.bfloat16)
    residual_wide = residual.astype(jnp.float32)
    ffn_in = (residual_wide * inverse_rms(lax.optimization_barrier(jnp.sum(residual_wide * residual_wide, axis=1, keepdims=True)), D) * ffn_gain.astype(jnp.float32)).astype(jnp.bfloat16)
    flat_ids = expert_ids.reshape(N_EP, SEQ_DEV * TOPK)
    choose = (flat_ids[:, :, None] == jnp.arange(EXPERTS, dtype=jnp.int32)[None, None, :]).astype(jnp.int32)
    earlier = jnp.cumsum(choose, axis=1) - choose
    slot_of = lax.optimization_barrier(jnp.sum(earlier * choose, axis=2))
    source = jnp.broadcast_to(jnp.arange(N_EP, dtype=jnp.int32)[:, None], slot_of.shape)
    token_of = source * SEQ_DEV + jnp.broadcast_to((jnp.arange(SEQ_DEV * TOPK, dtype=jnp.int32) // TOPK)[None, :], slot_of.shape)
    row_table = jnp.full((EXPERTS, N_EP, CAP), TOKENS, jnp.int32).at[flat_ids, source, slot_of].set(token_of)
    padded = jnp.concatenate([ffn_in, jnp.zeros((1, D), jnp.bfloat16)], axis=0)

    def one_expert(expert):
        expert_rows = padded[row_table[expert].reshape(-1)]
        gate_act = jnp.dot(expert_rows, gate_experts[expert], preferred_element_type=jnp.float32)
        up_act = jnp.dot(expert_rows, up_experts[expert], preferred_element_type=jnp.float32)
        active = (jax.nn.silu(gate_act) * up_act).astype(jnp.bfloat16)
        return jnp.dot(active, down_experts[expert], preferred_element_type=jnp.float32).astype(jnp.bfloat16)
    outputs = lax.map(one_expert, jnp.arange(EXPERTS, dtype=jnp.int32))
    where_row = (source * CAP + slot_of).reshape(TOKENS, TOPK)
    picked = outputs[expert_ids, where_row].astype(jnp.float32)
    route_weight = jax.nn.softmax(route_logits.astype(jnp.float32), axis=1)
    combined = lax.optimization_barrier(jnp.sum(route_weight[:, :, None] * picked, axis=1))
    result = residual_wide + combined * inverse_rms(lax.optimization_barrier(jnp.sum(combined * combined, axis=1, keepdims=True)), D) * out_gain.astype(jnp.float32)
    return result.astype(jnp.bfloat16)
```

```python
import functools

import jax
import jax.numpy as jnp
from jax import lax
from jax.experimental import pallas as pl
from jax.experimental.pallas import tpu as pltpu
from jax.sharding import PartitionSpec as P

epsilon = 1e-06
f32 = jnp.float32
bf16 = jnp.bfloat16

VMEM = pl.BlockSpec(memory_space=pltpu.VMEM)
SMEM = pl.BlockSpec(memory_space=pltpu.SMEM)


def inverse_rms(wide):
    return lax.rsqrt(jnp.sum(wide * wide, axis=1, keepdims=True) / wide.shape[1] + epsilon)


def swap(array, axis, offset):
    count = lax.axis_size(axis)
    return lax.ppermute(array, axis, [(i, i ^ offset) for i in range(count)])


def norm_body(hidden_ref, gain_ref, out_ref):
    wide = hidden_ref[...].astype(f32)
    normed = (wide * inverse_rms(wide) * gain_ref[...].astype(f32)).astype(bf16)
    parts, rows, width = out_ref.shape
    spare = rows - normed.shape[0]
    if spare:
        normed = jnp.concatenate([normed, jnp.zeros((spare, normed.shape[1]), bf16)], axis=0)
    for part in range(parts):
        out_ref[part] = normed[:, part * width : (part + 1) * width]


def project_body(rows_ref, weight_ref, out_ref):
    parts, rows, width = rows_ref.shape
    flat = rows_ref[...].reshape(parts * rows, width)
    out = jnp.dot(flat, weight_ref[...], preferred_element_type=f32)
    out_ref[...] = out.astype(bf16).reshape(out_ref.shape)


def attend_body(heads, lengths_ref, bias_ref, partial_ref, key_ref, value_ref, out_ref, query_ref):
    step = pl.program_id(0)
    group, columns, positions = key_ref.shape
    head_size = columns // heads

    @pl.when(step == 0)
    def _():
        total = jnp.sum(partial_ref[...].astype(f32), axis=0)
        query_ref[...] = total.astype(bf16).astype(f32)

    rows = group * heads
    head_of = lax.broadcasted_iota(jnp.int32, (heads, columns), 1) // head_size
    own_head = head_of == lax.broadcasted_iota(jnp.int32, (heads, columns), 0)
    scores = []
    for g in range(group):
        query = query_ref[pl.ds(step * group + g, 1), :]
        spread = jnp.where(own_head, query, 0.0).astype(bf16)
        scores.append(jnp.dot(spread, key_ref[g], preferred_element_type=f32))
    scores = jnp.concatenate(scores, axis=0)
    row = lax.broadcasted_iota(jnp.int32, (rows, positions), 0)
    bias = jnp.zeros((rows, positions), f32)
    length = jnp.zeros((rows, positions), jnp.int32)
    for h in range(heads):
        bias = jnp.where(row % heads == h, bias_ref[h], bias)
    for g in range(group):
        length = jnp.where(row // heads == g, lengths_ref[step * group + g], length)
    scores = scores * head_size ** (-0.5) + bias
    inside = lax.broadcasted_iota(jnp.int32, (rows, positions), 1) < length
    tail = jnp.log1p(jnp.exp(-jnp.abs(scores)))
    log_fail = jnp.where(inside, -jnp.maximum(scores, 0.0) - tail, 0.0)
    log_stick = jnp.minimum(scores, 0.0) - tail
    lane = 128
    blocks = positions // lane
    later = (
        lax.broadcasted_iota(jnp.int32, (lane, lane), 0)
        > lax.broadcasted_iota(jnp.int32, (lane, lane), 1)
    ).astype(f32)
    stacked = jnp.concatenate([log_fail[:, k * lane : (k + 1) * lane] for k in range(blocks)], axis=0)
    within = jnp.dot(stacked, later, preferred_element_type=f32, precision=lax.Precision.HIGHEST)
    totals = jnp.sum(stacked, axis=1, keepdims=True)
    carry = jnp.zeros((rows, 1), f32)
    after = [None] * blocks
    for k in reversed(range(blocks)):
        after[k] = within[k * rows : (k + 1) * rows] + carry
        carry = carry + totals[k * rows : (k + 1) * rows]
    after = jnp.concatenate(after, axis=1)
    weight = jnp.where(inside, jnp.exp(log_stick + after), 0.0).astype(bf16)
    for g in range(group):
        every = lax.dot_general(
            weight[g * heads : (g + 1) * heads],
            value_ref[g],
            (((1,), (1,)), ((), ())),
            preferred_element_type=f32,
        )
        mixed = jnp.sum(jnp.where(own_head, every, 0.0), axis=0, keepdims=True)
        out_ref[pl.ds(step * group + g, 1), :] = mixed.astype(bf16).astype(f32)


def out_body(aligned, place_ref, mixed_ref, *refs):
    out_ref = refs[-1]
    mixed = mixed_ref[...].astype(bf16)
    width = refs[0].shape[1]
    for offset, piece in enumerate(refs[:-1]):
        part = jnp.dot(mixed, piece[...], preferred_element_type=f32).astype(bf16)
        if aligned:
            start = pl.multiple_of((place_ref[0] ^ offset) * width, width)
            out_ref[:, pl.ds(start, width)] = part
        else:
            out_ref[offset] = part


def placings(ids, slots, capacity, experts):
    sequences, picks = ids.shape
    earlier = (
        lax.broadcasted_iota(jnp.int32, (sequences, sequences), 0)
        > lax.broadcasted_iota(jnp.int32, (sequences, sequences), 1)
    ).astype(f32)
    used = jnp.zeros((1, experts), f32)
    out = []
    for k in range(picks):
        column = ids[:, k : k + 1]
        chosen = (lax.broadcasted_iota(jnp.int32, (sequences, experts), 1) == column).astype(f32)
        before = jnp.dot(earlier, chosen, preferred_element_type=f32) + used
        slot = jnp.sum(before * chosen, axis=1, keepdims=True).astype(jnp.int32)
        used = used + jnp.sum(chosen, axis=0, keepdims=True)
        target = column * capacity + slot
        out.append(lax.broadcasted_iota(jnp.int32, (sequences, slots), 1) == target)
    return out


def residual_body(capacity, experts, ids_ref, hidden_ref, post_ref, ffn_ref, *refs):
    *partials, residual_ref, out_ref = refs
    total = partials[0][...].astype(f32)
    for partial in partials[1:]:
        total = total + partial[...].astype(f32)
    attended = total.astype(bf16).astype(f32)
    residual = (
        hidden_ref[...].astype(f32) + attended * inverse_rms(attended) * post_ref[...].astype(f32)
    ).astype(bf16)
    residual_ref[...] = residual
    wide = residual.astype(f32)
    ffn_in = (wide * inverse_rms(wide) * ffn_ref[...].astype(f32)).astype(bf16)
    slots = experts * capacity
    chosen = functools.reduce(jnp.logical_or, placings(ids_ref[...], slots, capacity, experts))
    outgoing = lax.dot_general(
        chosen.astype(f32).astype(bf16), ffn_in, (((0,), (0,)), ((), ())), preferred_element_type=f32
    )
    out_ref[...] = outgoing.astype(bf16).reshape(out_ref.shape)


def expert_body(rows_ref, gate_ref, up_ref, down_ref, out_ref, sum_ref):
    step = pl.program_id(0)
    sources, capacity, features = rows_ref.shape
    rows = rows_ref[...].reshape(sources * capacity, features)
    gate = jnp.dot(rows, gate_ref[...], preferred_element_type=f32)
    up = jnp.dot(rows, up_ref[...], preferred_element_type=f32)
    active = (gate / (1.0 + jnp.exp(-gate)) * up).astype(bf16)
    part = jnp.dot(active, down_ref[...], preferred_element_type=f32)

    @pl.when(step == 0)
    def _():
        sum_ref[...] = part

    @pl.when(step > 0)
    def _():
        sum_ref[...] = sum_ref[...] + part

    @pl.when(step == pl.num_programs(0) - 1)
    def _():
        width = out_ref.shape[3]
        for t in range(out_ref.shape[1]):
            piece = sum_ref[:, t * width : (t + 1) * width].astype(bf16)
            out_ref[:, t] = piece.reshape(sources, capacity, width)


def combine_body(capacity, experts, ids_ref, logits_ref, table_ref, combined_ref, squares_ref):
    homes, parts, rows, width = table_ref.shape
    total = table_ref[:, 0].astype(f32)
    for t in range(1, parts):
        total = total + table_ref[:, t].astype(f32)
    table = total.astype(bf16).reshape(homes * rows, width)
    logits = logits_ref[...]
    logits = jnp.exp(logits - jnp.max(logits, axis=1, keepdims=True))
    route = logits / jnp.sum(logits, axis=1, keepdims=True)
    combined = 0.0
    for k, placed in enumerate(placings(ids_ref[...], homes * rows, capacity, experts)):
        picked = jnp.dot(placed.astype(f32).astype(bf16), table, preferred_element_type=f32)
        combined = combined + route[:, k : k + 1] * picked
    combined_ref[...] = combined
    squares = jnp.sum(combined * combined, axis=1, keepdims=True)
    squares_ref[...] = jnp.broadcast_to(squares, squares_ref.shape)


def finish_body(features, place_ref, residual_ref, combined_ref, gain_ref, *refs):
    *squares_refs, out_ref = refs
    squares = squares_refs[0][...]
    for ref in squares_refs[1:]:
        squares = squares + ref[...]
    scale = lax.rsqrt(squares[:, :1] / features + epsilon)
    out = residual_ref[...].astype(f32) + combined_ref[...] * scale * gain_ref[...].astype(f32)
    out_ref[...] = out.astype(bf16)


def per_device(
    hidden,
    pre_gain,
    query_weight,
    key_cache,
    value_cache,
    lengths,
    stick_bias,
    out_weight,
    post_gain,
    ffn_gain,
    expert_ids,
    route_logits,
    gate_experts,
    up_experts,
    down_experts,
    out_gain,
):
    sequences, features = hidden.shape
    ep_count = lax.axis_size("ep")
    tp_count = lax.axis_size("tp")
    ep_place = lax.axis_index("ep").astype(jnp.int32).reshape(1)
    tp_place = lax.axis_index("tp").astype(jnp.int32).reshape(1)
    heads_here = stick_bias.shape[0]
    columns, positions = key_cache.shape[1:]
    shape = jax.ShapeDtypeStruct
    padded = -(-sequences // 16) * 16

    even = {0: out_weight}
    for offset in range(2, ep_count, 2):
        even[offset] = swap(out_weight, "ep", offset)

    chunk = features // ep_count
    normed = pl.pallas_call(
        norm_body,
        out_shape=shape((ep_count, padded, chunk), bf16),
        in_specs=[VMEM] * 2,
        out_specs=VMEM,
        name="norm",
    )(hidden, pre_gain.reshape(1, features))
    gathered = lax.all_to_all(normed, "ep", 0, 0, tiled=True)
    partial = pl.pallas_call(
        project_body,
        out_shape=shape((ep_count, padded, columns), bf16),
        in_specs=[VMEM] * 2,
        out_specs=VMEM,
        name="project",
    )(gathered, query_weight)
    partial = lax.all_to_all(partial, "ep", 0, 0, tiled=True)

    odd = {offset + 1: swap(piece, "ep", 1) for offset, piece in even.items()}
    pieces = {**even, **odd}

    group = 2 if sequences % 2 == 0 else 1
    mixed = pl.pallas_call(
        functools.partial(attend_body, heads_here),
        out_shape=shape((sequences, columns), f32),
        grid=(sequences // group,),
        in_specs=[
            SMEM,
            SMEM,
            pl.BlockSpec((ep_count, padded, columns), lambda i: (0, 0, 0)),
            pl.BlockSpec((group, columns, positions), lambda i: (i, 0, 0)),
            pl.BlockSpec((group, columns, positions), lambda i: (i, 0, 0)),
        ],
        out_specs=pl.BlockSpec((sequences, columns), lambda i: (0, 0)),
        scratch_shapes=[pltpu.VMEM((padded, columns), f32)],
        name="attend",
    )(lengths, stick_bias, partial, key_cache, value_cache)

    width = out_weight.shape[1]
    aligned = width % 128 == 0
    projected = pl.pallas_call(
        functools.partial(out_body, aligned),
        out_shape=shape((sequences, features) if aligned else (ep_count, sequences, width), bf16),
        in_specs=[SMEM] + [VMEM] * (1 + ep_count),
        out_specs=VMEM,
        name="outward",
    )(ep_place, mixed, *[pieces[offset] for offset in range(ep_count)])
    if not aligned:
        projected = jnp.take(projected, ep_place ^ jnp.arange(ep_count), axis=0)
        projected = projected.transpose(1, 0, 2).reshape(sequences, features)
    partials = [projected] + [swap(projected, "tp", offset) for offset in range(1, tp_count)]

    pick_count = expert_ids.shape[1]
    local_experts = gate_experts.shape[0]
    experts = local_experts * ep_count
    capacity = max(2, (2 * pick_count * sequences + experts - 1) // experts)
    capacity = -(-capacity // 8) * 8
    residual, outgoing = pl.pallas_call(
        functools.partial(residual_body, capacity, experts),
        out_shape=(
            shape((sequences, features), bf16),
            shape((experts, capacity, features), bf16),
        ),
        in_specs=[VMEM] * (4 + tp_count),
        out_specs=(VMEM, VMEM),
        name="residual",
    )(
        expert_ids,
        hidden,
        post_gain.reshape(1, features),
        ffn_gain.reshape(1, features),
        *partials,
    )
    arrived = lax.all_to_all(outgoing, "ep", 0, 0, tiled=True)
    arrived = arrived.reshape(ep_count, local_experts, capacity, features)

    hidden_units = gate_experts.shape[2]
    slice_width = features // tp_count
    block = min(hidden_units, 256)
    results = []
    for own in range(local_experts):
        results.append(
            pl.pallas_call(
                expert_body,
                out_shape=shape((ep_count, tp_count, capacity, slice_width), bf16),
                grid=(hidden_units // block,),
                in_specs=[
                    pl.BlockSpec((ep_count, capacity, features), lambda i: (0, 0, 0)),
                    pl.BlockSpec((features, block), lambda i: (0, i)),
                    pl.BlockSpec((features, block), lambda i: (0, i)),
                    pl.BlockSpec((block, features), lambda i: (i, 0)),
                ],
                out_specs=pl.BlockSpec(
                    (ep_count, tp_count, capacity, slice_width), lambda i: (0, 0, 0, 0)
                ),
                scratch_shapes=[pltpu.VMEM((ep_count * capacity, features), f32)],
                name="expert",
            )(arrived[:, own], gate_experts[own], up_experts[own], down_experts[own])
        )
    partial_out = results[0] if local_experts == 1 else jnp.concatenate(results, axis=2)
    rows = local_experts * capacity
    flat = partial_out.reshape(ep_count * tp_count, rows, slice_width)
    returned = lax.all_to_all(flat, ("ep", "tp"), 0, 0, tiled=True)
    table = returned.reshape(ep_count, tp_count, rows, slice_width)
    combined, squares = pl.pallas_call(
        functools.partial(combine_body, capacity, experts),
        out_shape=(shape((sequences, slice_width), f32), shape((sequences, 128), f32)),
        in_specs=[VMEM] * 3,
        out_specs=(VMEM, VMEM),
        name="combine",
    )(expert_ids, route_logits, table)
    every = [squares] + [swap(squares, "tp", offset) for offset in range(1, tp_count)]
    own_slice = lambda i, place: (0, place[0])
    whole = lambda i, place: (0, 0)
    return pl.pallas_call(
        functools.partial(finish_body, features),
        out_shape=shape((sequences, slice_width), bf16),
        grid_spec=pltpu.PrefetchScalarGridSpec(
            num_scalar_prefetch=1,
            grid=(1,),
            in_specs=[
                pl.BlockSpec((sequences, slice_width), own_slice),
                pl.BlockSpec((sequences, slice_width), whole),
                pl.BlockSpec((1, slice_width), whole),
            ]
            + [pl.BlockSpec((sequences, 128), whole)] * tp_count,
            out_specs=pl.BlockSpec((sequences, slice_width), whole),
        ),
        name="finish",
    )(tp_place, residual, combined, out_gain.reshape(1, slice_width), *every)


def solution(mesh):
    placed = (
        P("ep", None),
        P(),
        P("ep", "tp"),
        P("ep", "tp", None),
        P("ep", "tp", None),
        P("ep"),
        P("tp"),
        P("tp", "ep"),
        P(),
        P(),
        P("ep", None),
        P("ep", None),
        P("ep", None, "tp"),
        P("ep", None, "tp"),
        P("ep", "tp", None),
        P("tp"),
    )
    return jax.shard_map(
        per_device, mesh=mesh, in_specs=placed, out_specs=P("ep", "tp"), check_vma=False
    )
```

```python
import functools

import jax
import jax.numpy as jnp
from jax import lax
from jax.experimental import pallas as pl
from jax.experimental.pallas import tpu as pltpu
from jax.sharding import PartitionSpec as P

epsilon = 1e-06
f32 = jnp.float32
bf16 = jnp.bfloat16

VMEM = pl.BlockSpec(memory_space=pltpu.VMEM)
HBM = pl.BlockSpec(memory_space=pltpu.HBM)
SMEM = pl.BlockSpec(memory_space=pltpu.SMEM)


GRANT = pltpu.CompilerParams(vmem_limit_bytes=32 * 1024 * 1024)


def near(*arrays):
    return [pltpu.with_memory_space_constraint(array, pltpu.VMEM) for array in arrays]


def far(*arrays):
    return [pltpu.with_memory_space_constraint(array, pltpu.HBM) for array in arrays]


def made(shape, dtype):
    return pltpu.VMEM(shape, dtype)


def inverse_rms(wide):
    return lax.rsqrt(jnp.sum(wide * wide, axis=1, keepdims=True) / wide.shape[1] + epsilon)


def swap(array, axis, offset):
    count = lax.axis_size(axis)
    return lax.ppermute(array, axis, [(i, i ^ offset) for i in range(count)])


def norm_body(hidden_ref, gain_ref, out_ref):
    wide = hidden_ref[...].astype(f32)
    normed = (wide * inverse_rms(wide) * gain_ref[...].astype(f32)).astype(bf16)
    parts, rows, width = out_ref.shape
    spare = rows - normed.shape[0]
    if spare:
        normed = jnp.concatenate([normed, jnp.zeros((spare, normed.shape[1]), bf16)], axis=0)
    for part in range(parts):
        out_ref[part] = normed[:, part * width : (part + 1) * width]


def project_body(rows_ref, weight_ref, out_ref):
    parts, rows, width = rows_ref.shape
    flat = rows_ref[...].reshape(parts * rows, width)
    out = jnp.dot(flat, weight_ref[...], preferred_element_type=f32)
    out_ref[...] = out.astype(bf16).reshape(out_ref.shape)


def attend_body(
    heads,
    group,
    lengths_ref,
    bias_ref,
    partial_ref,
    key_far,
    value_far,
    out_ref,
    query_ref,
    key_ref,
    value_ref,
    sems,
):
    sequences, columns, positions = key_ref.shape
    copies = []
    for step in range(sequences // group):
        part = pl.ds(step * group, group)
        copies.append(
            (
                pltpu.make_async_copy(key_far.at[part], key_ref.at[part], sems.at[0, step]),
                pltpu.make_async_copy(value_far.at[part], value_ref.at[part], sems.at[1, step]),
            )
        )
        copies[-1][0].start()
        copies[-1][1].start()
    head_size = columns // heads
    total = jnp.sum(partial_ref[...].astype(f32), axis=0)
    query_ref[...] = total.astype(bf16).astype(f32)
    rows = group * heads
    head_of = lax.broadcasted_iota(jnp.int32, (heads, columns), 1) // head_size
    own_head = head_of == lax.broadcasted_iota(jnp.int32, (heads, columns), 0)
    row = lax.broadcasted_iota(jnp.int32, (rows, positions), 0)
    bias = jnp.zeros((rows, positions), f32)
    for h in range(heads):
        bias = jnp.where(row % heads == h, bias_ref[h], bias)
    lane = 128
    blocks = positions // lane
    later = (
        lax.broadcasted_iota(jnp.int32, (lane, lane), 0)
        > lax.broadcasted_iota(jnp.int32, (lane, lane), 1)
    ).astype(f32)
    for first in range(0, sequences, group):
        scores = []
        length = jnp.zeros((rows, positions), jnp.int32)
        copies[first // group][0].wait()
        for g in range(group):
            query = query_ref[first + g : first + g + 1, :]
            spread = jnp.where(own_head, query, 0.0).astype(bf16)
            scores.append(jnp.dot(spread, key_ref[first + g], preferred_element_type=f32))
            length = jnp.where(row // heads == g, lengths_ref[first + g], length)
        scores = jnp.concatenate(scores, axis=0)
        scores = scores * head_size ** (-0.5) + bias
        inside = lax.broadcasted_iota(jnp.int32, (rows, positions), 1) < length
        tail = jnp.log1p(jnp.exp(-jnp.abs(scores)))
        log_fail = jnp.where(inside, -jnp.maximum(scores, 0.0) - tail, 0.0)
        log_stick = jnp.minimum(scores, 0.0) - tail
        stacked = jnp.concatenate(
            [log_fail[:, k * lane : (k + 1) * lane] for k in range(blocks)], axis=0
        )
        within = jnp.dot(
            stacked, later, preferred_element_type=f32, precision=lax.Precision.HIGHEST
        )
        totals = jnp.sum(stacked, axis=1, keepdims=True)
        carry = jnp.zeros((rows, 1), f32)
        after = [None] * blocks
        for k in reversed(range(blocks)):
            after[k] = within[k * rows : (k + 1) * rows] + carry
            carry = carry + totals[k * rows : (k + 1) * rows]
        after = jnp.concatenate(after, axis=1)
        weight = jnp.where(inside, jnp.exp(log_stick + after), 0.0).astype(bf16)
        copies[first // group][1].wait()
        for g in range(group):
            every = lax.dot_general(
                weight[g * heads : (g + 1) * heads],
                value_ref[first + g],
                (((1,), (1,)), ((), ())),
                preferred_element_type=f32,
            )
            mixed = jnp.sum(jnp.where(own_head, every, 0.0), axis=0, keepdims=True)
            out_ref[first + g : first + g + 1, :] = mixed.astype(bf16).astype(f32)


def out_body(aligned, place_ref, mixed_ref, *refs):
    out_ref = refs[-1]
    mixed = mixed_ref[...].astype(bf16)
    width = refs[0].shape[1]
    for offset, piece in enumerate(refs[:-1]):
        part = jnp.dot(mixed, piece[...], preferred_element_type=f32).astype(bf16)
        if aligned:
            start = pl.multiple_of((place_ref[0] ^ offset) * width, width)
            out_ref[:, pl.ds(start, width)] = part
        else:
            out_ref[offset] = part


def placings(ids, slots, capacity, experts):
    sequences, picks = ids.shape
    earlier = (
        lax.broadcasted_iota(jnp.int32, (sequences, sequences), 0)
        > lax.broadcasted_iota(jnp.int32, (sequences, sequences), 1)
    ).astype(f32)
    used = jnp.zeros((1, experts), f32)
    out = []
    for k in range(picks):
        column = ids[:, k : k + 1]
        chosen = (lax.broadcasted_iota(jnp.int32, (sequences, experts), 1) == column).astype(f32)
        before = jnp.dot(earlier, chosen, preferred_element_type=f32) + used
        slot = jnp.sum(before * chosen, axis=1, keepdims=True).astype(jnp.int32)
        used = used + jnp.sum(chosen, axis=0, keepdims=True)
        target = column * capacity + slot
        out.append(lax.broadcasted_iota(jnp.int32, (sequences, slots), 1) == target)
    return out


def residual_body(capacity, experts, ids_ref, hidden_ref, post_ref, ffn_ref, *refs):
    *partials, residual_ref, out_ref = refs
    total = partials[0][...].astype(f32)
    for partial in partials[1:]:
        total = total + partial[...].astype(f32)
    attended = total.astype(bf16).astype(f32)
    residual = (
        hidden_ref[...].astype(f32) + attended * inverse_rms(attended) * post_ref[...].astype(f32)
    ).astype(bf16)
    residual_ref[...] = residual
    wide = residual.astype(f32)
    ffn_in = (wide * inverse_rms(wide) * ffn_ref[...].astype(f32)).astype(bf16)
    slots = experts * capacity
    chosen = functools.reduce(jnp.logical_or, placings(ids_ref[...], slots, capacity, experts))
    outgoing = lax.dot_general(
        chosen.astype(f32).astype(bf16), ffn_in, (((0,), (0,)), ((), ())), preferred_element_type=f32
    )
    out_ref[...] = outgoing.astype(bf16).reshape(out_ref.shape)


def expert_body(rows_ref, gate_far, up_far, down_far, out_ref, gate_ref, up_ref, down_ref, sems):
    ends = ((gate_far, gate_ref), (up_far, up_ref), (down_far, down_ref))
    copies = [pltpu.make_async_copy(*pair, sems.at[i]) for i, pair in enumerate(ends)]
    for copy in copies:
        copy.start()
    sources, capacity, features = rows_ref.shape
    rows = rows_ref[...].reshape(sources * capacity, features)
    copies[0].wait()
    gate = jnp.dot(rows, gate_ref[...], preferred_element_type=f32)
    copies[1].wait()
    up = jnp.dot(rows, up_ref[...], preferred_element_type=f32)
    active = (gate / (1.0 + jnp.exp(-gate)) * up).astype(bf16)
    width = out_ref.shape[3]
    copies[2].wait()
    for t in range(out_ref.shape[1]):
        down = down_ref[:, t * width : (t + 1) * width]
        part = jnp.dot(active, down, preferred_element_type=f32).astype(bf16)
        out_ref[:, t] = part.reshape(sources, capacity, width)


def combine_body(capacity, experts, ids_ref, logits_ref, table_ref, combined_ref, squares_ref):
    homes, parts, rows, width = table_ref.shape
    total = table_ref[:, 0].astype(f32)
    for t in range(1, parts):
        total = total + table_ref[:, t].astype(f32)
    table = total.astype(bf16).reshape(homes * rows, width)
    logits = logits_ref[...]
    logits = jnp.exp(logits - jnp.max(logits, axis=1, keepdims=True))
    route = logits / jnp.sum(logits, axis=1, keepdims=True)
    combined = 0.0
    for k, placed in enumerate(placings(ids_ref[...], homes * rows, capacity, experts)):
        picked = jnp.dot(placed.astype(f32).astype(bf16), table, preferred_element_type=f32)
        combined = combined + route[:, k : k + 1] * picked
    combined_ref[...] = combined
    squares = jnp.sum(combined * combined, axis=1, keepdims=True)
    squares_ref[...] = jnp.broadcast_to(squares, squares_ref.shape)


def finish_body(features, place_ref, residual_ref, combined_ref, gain_ref, *refs):
    *squares_refs, out_ref = refs
    squares = squares_refs[0][...]
    for ref in squares_refs[1:]:
        squares = squares + ref[...]
    scale = lax.rsqrt(squares[:, :1] / features + epsilon)
    width = out_ref.shape[1]
    start = pl.multiple_of(place_ref[0] * width, width)
    residual = residual_ref[:, pl.ds(start, width)].astype(f32)
    out = residual + combined_ref[...] * scale * gain_ref[...].astype(f32)
    out_ref[...] = out.astype(bf16)


def per_device(
    hidden,
    pre_gain,
    query_weight,
    key_cache,
    value_cache,
    lengths,
    stick_bias,
    out_weight,
    post_gain,
    ffn_gain,
    expert_ids,
    route_logits,
    gate_experts,
    up_experts,
    down_experts,
    out_gain,
):
    sequences, features = hidden.shape
    ep_count = lax.axis_size("ep")
    tp_count = lax.axis_size("tp")
    ep_place = lax.axis_index("ep").astype(jnp.int32).reshape(1)
    tp_place = lax.axis_index("tp").astype(jnp.int32).reshape(1)
    heads_here = stick_bias.shape[0]
    columns, positions = key_cache.shape[1:]
    padded = -(-sequences // 16) * 16

    chunk = features // ep_count
    normed = pl.pallas_call(
        norm_body,
        out_shape=made((ep_count, padded, chunk), bf16),
        in_specs=[VMEM] * 2,
        out_specs=VMEM,
        name="norm",
        compiler_params=GRANT,
    )(*near(hidden, pre_gain.reshape(1, features)))
    normed, out_weight = lax.optimization_barrier((normed, out_weight))
    even = {0: out_weight}
    for offset in range(2, ep_count, 2):
        even[offset] = swap(out_weight, "ep", offset)
    gathered = lax.all_to_all(normed, "ep", 0, 0, tiled=True)
    partial = pl.pallas_call(
        project_body,
        out_shape=made((ep_count, padded, columns), bf16),
        in_specs=[VMEM] * 2,
        out_specs=VMEM,
        name="project",
        compiler_params=GRANT,
    )(*near(gathered, query_weight))
    partial = lax.all_to_all(partial, "ep", 0, 0, tiled=True)

    odd = {offset + 1: swap(piece, "ep", 1) for offset, piece in even.items()}
    pieces = {**even, **odd}

    group = 2 if sequences % 2 == 0 else 1
    mixed = pl.pallas_call(
        functools.partial(attend_body, heads_here, group),
        out_shape=made((sequences, columns), f32),
        in_specs=[SMEM, SMEM, VMEM, HBM, HBM],
        out_specs=VMEM,
        scratch_shapes=[
            pltpu.VMEM((padded, columns), f32),
            pltpu.VMEM(key_cache.shape, bf16),
            pltpu.VMEM(value_cache.shape, bf16),
            pltpu.SemaphoreType.DMA((2, sequences // group)),
        ],
        name="attend",
        compiler_params=GRANT,
    )(lengths, stick_bias, *near(partial), *far(key_cache, value_cache))

    width = out_weight.shape[1]
    aligned = width % 128 == 0
    projected = pl.pallas_call(
        functools.partial(out_body, aligned),
        out_shape=made((sequences, features) if aligned else (ep_count, sequences, width), bf16),
        in_specs=[SMEM] + [VMEM] * (1 + ep_count),
        out_specs=VMEM,
        name="outward",
        compiler_params=GRANT,
    )(ep_place, *near(mixed, *[pieces[offset] for offset in range(ep_count)]))
    if not aligned:
        projected = jnp.take(projected, ep_place ^ jnp.arange(ep_count), axis=0)
        projected = projected.transpose(1, 0, 2).reshape(sequences, features)
    partials = [projected] + [swap(projected, "tp", offset) for offset in range(1, tp_count)]

    pick_count = expert_ids.shape[1]
    local_experts = gate_experts.shape[0]
    experts = local_experts * ep_count
    capacity = max(2, (2 * pick_count * sequences + experts - 1) // experts)
    capacity = -(-capacity // 8) * 8
    residual, outgoing = pl.pallas_call(
        functools.partial(residual_body, capacity, experts),
        out_shape=(
            made((sequences, features), bf16),
            made((experts, capacity, features), bf16),
        ),
        in_specs=[VMEM] * (4 + tp_count),
        out_specs=(VMEM, VMEM),
        name="residual",
        compiler_params=GRANT,
    )(
        *near(
            expert_ids,
            hidden,
            post_gain.reshape(1, features),
            ffn_gain.reshape(1, features),
            *partials,
        )
    )
    arrived = lax.all_to_all(outgoing, "ep", 0, 0, tiled=True)
    arrived = arrived.reshape(ep_count, local_experts, capacity, features)

    slice_width = features // tp_count
    results = []
    for own in range(local_experts):
        weights = (gate_experts[own], up_experts[own], down_experts[own])
        results.append(
            pl.pallas_call(
                expert_body,
                out_shape=made((ep_count, tp_count, capacity, slice_width), bf16),
                in_specs=[VMEM] + [HBM] * 3,
                out_specs=VMEM,
                scratch_shapes=[pltpu.VMEM(array.shape, bf16) for array in weights]
                + [pltpu.SemaphoreType.DMA((3,))],
                name="expert",
                compiler_params=GRANT,
            )(*near(arrived[:, own]), *far(*weights))
        )
    partial_out = results[0] if local_experts == 1 else jnp.concatenate(results, axis=2)
    rows = local_experts * capacity
    flat = partial_out.reshape(ep_count * tp_count, rows, slice_width)
    returned = lax.all_to_all(flat, ("ep", "tp"), 0, 0, tiled=True)
    table = returned.reshape(ep_count, tp_count, rows, slice_width)
    combined, squares = pl.pallas_call(
        functools.partial(combine_body, capacity, experts),
        out_shape=(made((sequences, slice_width), f32), made((sequences, 128), f32)),
        in_specs=[VMEM] * 3,
        out_specs=(VMEM, VMEM),
        name="combine",
        compiler_params=GRANT,
    )(*near(expert_ids, route_logits, table))
    every = [squares] + [swap(squares, "tp", offset) for offset in range(1, tp_count)]
    return pl.pallas_call(
        functools.partial(finish_body, features),
        out_shape=jax.ShapeDtypeStruct((sequences, slice_width), bf16),
        in_specs=[SMEM] + [VMEM] * (3 + tp_count),
        out_specs=VMEM,
        name="finish",
        compiler_params=GRANT,
    )(tp_place, *near(residual, combined, out_gain.reshape(1, slice_width), *every))


def solution(mesh):
    placed = (
        P("ep", None),
        P(),
        P("ep", "tp"),
        P("ep", "tp", None),
        P("ep", "tp", None),
        P("ep"),
        P("tp"),
        P("tp", "ep"),
        P(),
        P(),
        P("ep", None),
        P("ep", None),
        P("ep", None, "tp"),
        P("ep", None, "tp"),
        P("ep", "tp", None),
        P("tp"),
    )
    return jax.shard_map(
        per_device, mesh=mesh, in_specs=placed, out_specs=P("ep", "tp"), check_vma=False
    )
```

```python
import functools

import jax
import jax.numpy as jnp
from jax import lax
from jax.experimental import pallas as pl
from jax.experimental.pallas import tpu as pltpu
from jax.sharding import PartitionSpec as P


epsilon = 1e-06
f32 = jnp.float32
bf16 = jnp.bfloat16

VMEM = pl.BlockSpec(memory_space=pltpu.VMEM)
HBM = pl.BlockSpec(memory_space=pltpu.HBM)
SMEM = pl.BlockSpec(memory_space=pltpu.SMEM)


GRANT = pltpu.CompilerParams(vmem_limit_bytes=32 * 1024 * 1024)


def near(*arrays):
    return [pltpu.with_memory_space_constraint(array, pltpu.VMEM) for array in arrays]


def far(*arrays):
    return [pltpu.with_memory_space_constraint(array, pltpu.HBM) for array in arrays]


def made(shape, dtype):
    return pltpu.VMEM(shape, dtype)


def inverse_rms(wide):
    return lax.rsqrt(jnp.sum(wide * wide, axis=1, keepdims=True) / wide.shape[1] + epsilon)


def swap(array, axis, offset):
    count = lax.axis_size(axis)
    return lax.ppermute(array, axis, [(i, i ^ offset) for i in range(count)])


def norm_body(hidden_far, gain_ref, weight_far, out_ref, weight_ref, hidden_ref, sems):
    first = pltpu.make_async_copy(hidden_far, hidden_ref, sems.at[0])
    second = pltpu.make_async_copy(weight_far, weight_ref, sems.at[1])
    first.start()
    second.start()
    first.wait()
    wide = hidden_ref[...].astype(f32)
    normed = (wide * inverse_rms(wide) * gain_ref[...].astype(f32)).astype(bf16)
    parts, rows, width = out_ref.shape
    spare = rows - normed.shape[0]
    if spare:
        normed = jnp.concatenate([normed, jnp.zeros((spare, normed.shape[1]), bf16)], axis=0)
    for part in range(parts):
        out_ref[part] = normed[:, part * width : (part + 1) * width]
    second.wait()


def project_body(rows_ref, weight_ref, out_ref):
    parts, rows, width = rows_ref.shape
    flat = rows_ref[...].reshape(parts * rows, width)
    out = jnp.dot(flat, weight_ref[...], preferred_element_type=f32)
    out_ref[...] = out.astype(bf16).reshape(out_ref.shape)


def attend_body(
    heads,
    group,
    lengths_far,
    bias_far,
    partial_ref,
    key_far,
    value_far,
    out_ref,
    query_ref,
    key_ref,
    value_ref,
    sems,
    lengths_ref,
    bias_ref,
    small_sems,
):
    small = (
        pltpu.make_async_copy(lengths_far, lengths_ref, small_sems.at[0]),
        pltpu.make_async_copy(bias_far, bias_ref, small_sems.at[1]),
    )
    for copy in small:
        copy.start()
    sequences, columns, positions = key_ref.shape
    copies = []
    for step in range(sequences // group):
        part = pl.ds(step * group, group)
        copies.append(
            (
                pltpu.make_async_copy(key_far.at[part], key_ref.at[part], sems.at[0, step]),
                pltpu.make_async_copy(value_far.at[part], value_ref.at[part], sems.at[1, step]),
            )
        )
        copies[-1][0].start()
        copies[-1][1].start()
    head_size = columns // heads
    total = jnp.sum(partial_ref[...].astype(f32), axis=0)
    query_ref[...] = total.astype(bf16).astype(f32)
    rows = group * heads
    head_of = lax.broadcasted_iota(jnp.int32, (heads, columns), 1) // head_size
    own_head = head_of == lax.broadcasted_iota(jnp.int32, (heads, columns), 0)
    row = lax.broadcasted_iota(jnp.int32, (rows, positions), 0)
    bias = jnp.zeros((rows, positions), f32)
    for copy in small:
        copy.wait()
    for h in range(heads):
        bias = jnp.where(row % heads == h, bias_ref[h], bias)
    lane = 128
    blocks = positions // lane
    later = (
        lax.broadcasted_iota(jnp.int32, (lane, lane), 0)
        > lax.broadcasted_iota(jnp.int32, (lane, lane), 1)
    ).astype(f32)
    for first in range(0, sequences, group):
        scores = []
        length = jnp.zeros((rows, positions), jnp.int32)
        copies[first // group][0].wait()
        for g in range(group):
            query = query_ref[first + g : first + g + 1, :]
            spread = jnp.where(own_head, query, 0.0).astype(bf16)
            scores.append(jnp.dot(spread, key_ref[first + g], preferred_element_type=f32))
            length = jnp.where(row // heads == g, lengths_ref[first + g], length)
        scores = jnp.concatenate(scores, axis=0)
        scores = scores * head_size ** (-0.5) + bias
        inside = lax.broadcasted_iota(jnp.int32, (rows, positions), 1) < length
        tail = jnp.log1p(jnp.exp(-jnp.abs(scores)))
        log_fail = jnp.where(inside, -jnp.maximum(scores, 0.0) - tail, 0.0)
        log_stick = jnp.minimum(scores, 0.0) - tail
        stacked = jnp.concatenate(
            [log_fail[:, k * lane : (k + 1) * lane] for k in range(blocks)], axis=0
        )
        within = jnp.dot(
            stacked, later, preferred_element_type=f32, precision=lax.Precision.HIGHEST
        )
        totals = jnp.sum(stacked, axis=1, keepdims=True)
        carry = jnp.zeros((rows, 1), f32)
        after = [None] * blocks
        for k in reversed(range(blocks)):
            after[k] = within[k * rows : (k + 1) * rows] + carry
            carry = carry + totals[k * rows : (k + 1) * rows]
        after = jnp.concatenate(after, axis=1)
        weight = jnp.where(inside, jnp.exp(log_stick + after), 0.0).astype(bf16)
        copies[first // group][1].wait()
        for g in range(group):
            every = lax.dot_general(
                weight[g * heads : (g + 1) * heads],
                value_ref[first + g],
                (((1,), (1,)), ((), ())),
                preferred_element_type=f32,
            )
            mixed = jnp.sum(jnp.where(own_head, every, 0.0), axis=0, keepdims=True)
            out_ref[first + g : first + g + 1, :] = mixed.astype(bf16).astype(f32)


def out_body(aligned, place_ref, mixed_ref, *refs):
    out_ref = refs[-1]
    mixed = mixed_ref[...].astype(bf16)
    width = refs[0].shape[1]
    for offset, piece in enumerate(refs[:-1]):
        part = jnp.dot(mixed, piece[...], preferred_element_type=f32).astype(bf16)
        if aligned:
            start = pl.multiple_of((place_ref[0] ^ offset) * width, width)
            out_ref[:, pl.ds(start, width)] = part
        else:
            out_ref[offset] = part


def placings(ids, slots, capacity, experts):
    sequences, picks = ids.shape
    earlier = (
        lax.broadcasted_iota(jnp.int32, (sequences, sequences), 0)
        > lax.broadcasted_iota(jnp.int32, (sequences, sequences), 1)
    ).astype(f32)
    used = jnp.zeros((1, experts), f32)
    out = []
    for k in range(picks):
        column = ids[:, k : k + 1]
        chosen = (lax.broadcasted_iota(jnp.int32, (sequences, experts), 1) == column).astype(f32)
        before = jnp.dot(earlier, chosen, preferred_element_type=f32) + used
        slot = jnp.sum(before * chosen, axis=1, keepdims=True).astype(jnp.int32)
        used = used + jnp.sum(chosen, axis=0, keepdims=True)
        target = column * capacity + slot
        out.append(lax.broadcasted_iota(jnp.int32, (sequences, slots), 1) == target)
    return out


def residual_body(capacity, experts, ids_ref, hidden_ref, post_ref, ffn_ref, *refs):
    *partials, residual_ref, out_ref = refs
    total = partials[0][...].astype(f32)
    for partial in partials[1:]:
        total = total + partial[...].astype(f32)
    attended = total.astype(bf16).astype(f32)
    residual = (
        hidden_ref[...].astype(f32) + attended * inverse_rms(attended) * post_ref[...].astype(f32)
    ).astype(bf16)
    residual_ref[...] = residual
    wide = residual.astype(f32)
    ffn_in = (wide * inverse_rms(wide) * ffn_ref[...].astype(f32)).astype(bf16)
    slots = experts * capacity
    chosen = functools.reduce(jnp.logical_or, placings(ids_ref[...], slots, capacity, experts))
    outgoing = lax.dot_general(
        chosen.astype(f32).astype(bf16), ffn_in, (((0,), (0,)), ((), ())), preferred_element_type=f32
    )
    out_ref[...] = outgoing.astype(bf16).reshape(out_ref.shape)


def expert_body(rows_ref, gate_ref, up_far, down_far, out_ref, up_ref, down_ref, sems):
    ends = ((up_far, up_ref), (down_far, down_ref))
    copies = [pltpu.make_async_copy(*pair, sems.at[i]) for i, pair in enumerate(ends)]
    for copy in copies:
        copy.start()
    sources, capacity, features = rows_ref.shape
    rows = rows_ref[...].reshape(sources * capacity, features)
    gate = jnp.dot(rows, gate_ref[...], preferred_element_type=f32)
    copies[0].wait()
    up = jnp.dot(rows, up_ref[...], preferred_element_type=f32)
    active = (gate / (1.0 + jnp.exp(-gate)) * up).astype(bf16)
    width = out_ref.shape[3]
    copies[1].wait()
    for t in range(out_ref.shape[1]):
        down = down_ref[:, t * width : (t + 1) * width]
        part = jnp.dot(active, down, preferred_element_type=f32).astype(bf16)
        out_ref[:, t] = part.reshape(sources, capacity, width)


def combine_body(capacity, experts, ids_ref, logits_ref, table_ref, combined_ref, squares_ref):
    homes, parts, rows, width = table_ref.shape
    total = table_ref[:, 0].astype(f32)
    for t in range(1, parts):
        total = total + table_ref[:, t].astype(f32)
    table = total.astype(bf16).reshape(homes * rows, width)
    logits = logits_ref[...]
    logits = jnp.exp(logits - jnp.max(logits, axis=1, keepdims=True))
    route = logits / jnp.sum(logits, axis=1, keepdims=True)
    combined = 0.0
    for k, placed in enumerate(placings(ids_ref[...], homes * rows, capacity, experts)):
        picked = jnp.dot(placed.astype(f32).astype(bf16), table, preferred_element_type=f32)
        combined = combined + route[:, k : k + 1] * picked
    combined_ref[...] = combined
    squares = jnp.sum(combined * combined, axis=1, keepdims=True)
    squares_ref[...] = jnp.broadcast_to(squares, squares_ref.shape)


def finish_body(features, place_ref, residual_ref, combined_ref, gain_ref, *refs):
    *squares_refs, out_ref = refs
    squares = squares_refs[0][...]
    for ref in squares_refs[1:]:
        squares = squares + ref[...]
    scale = lax.rsqrt(squares[:, :1] / features + epsilon)
    width = out_ref.shape[1]
    start = pl.multiple_of(place_ref[0] * width, width)
    residual = residual_ref[:, pl.ds(start, width)].astype(f32)
    out = residual + combined_ref[...] * scale * gain_ref[...].astype(f32)
    out_ref[...] = out.astype(bf16)


def per_device(
    hidden,
    pre_gain,
    query_weight,
    key_cache,
    value_cache,
    lengths,
    stick_bias,
    out_weight,
    post_gain,
    ffn_gain,
    expert_ids,
    route_logits,
    gate_experts,
    up_experts,
    down_experts,
    out_gain,
):
    sequences, features = hidden.shape
    ep_count = lax.axis_size("ep")
    tp_count = lax.axis_size("tp")
    ep_place = lax.axis_index("ep").astype(jnp.int32).reshape(1)
    tp_place = lax.axis_index("tp").astype(jnp.int32).reshape(1)
    heads_here = stick_bias.shape[0]
    columns, _ = key_cache.shape[1:]
    if heads_here == 1:
        stick_bias = jnp.tile(stick_bias, 2)
    padded = -(-sequences // 16) * 16

    chunk = features // ep_count
    normed, near_weight = pl.pallas_call(
        norm_body,
        out_shape=(
            made((ep_count, padded, chunk), bf16),
            made(query_weight.shape, bf16),
        ),
        in_specs=[HBM, VMEM, HBM],
        out_specs=(VMEM, VMEM),
        scratch_shapes=[pltpu.VMEM(hidden.shape, bf16), pltpu.SemaphoreType.DMA((2,))],
        name="norm",
        compiler_params=GRANT,
    )(*far(hidden), *near(pre_gain.reshape(1, features)), *far(query_weight))
    gathered = lax.all_to_all(normed, "ep", 0, 0, tiled=True)
    even = {0: out_weight}
    for offset in range(2, ep_count, 2):
        even[offset] = swap(out_weight, "ep", offset)
    partial = pl.pallas_call(
        project_body,
        out_shape=made((ep_count, padded, columns), bf16),
        in_specs=[VMEM] * 2,
        out_specs=VMEM,
        name="project",
        compiler_params=GRANT,
    )(*near(gathered, near_weight))
    partial = lax.all_to_all(partial, "ep", 0, 0, tiled=True)

    odd = {offset + 1: swap(piece, "ep", 1) for offset, piece in even.items()}
    pieces = {**even, **odd}

    group = 2 if sequences % 2 == 0 else 1
    mixed = pl.pallas_call(
        functools.partial(attend_body, heads_here, group),
        out_shape=made((sequences, columns), f32),
        in_specs=[HBM, HBM, VMEM, HBM, HBM],
        out_specs=VMEM,
        scratch_shapes=[
            pltpu.VMEM((padded, columns), f32),
            pltpu.VMEM(key_cache.shape, bf16),
            pltpu.VMEM(value_cache.shape, bf16),
            pltpu.SemaphoreType.DMA((2, sequences // group)),
            pltpu.SMEM(lengths.shape, jnp.int32),
            pltpu.SMEM(stick_bias.shape, f32),
            pltpu.SemaphoreType.DMA((2,)),
        ],
        name="attend",
        compiler_params=GRANT,
    )(*far(lengths, stick_bias), *near(partial), *far(key_cache, value_cache))

    width = out_weight.shape[1]
    aligned = width % 128 == 0
    projected = pl.pallas_call(
        functools.partial(out_body, aligned),
        out_shape=made((sequences, features) if aligned else (ep_count, sequences, width), bf16),
        in_specs=[SMEM] + [VMEM] * (1 + ep_count),
        out_specs=VMEM,
        name="outward",
        compiler_params=GRANT,
    )(ep_place, *near(mixed, *[pieces[offset] for offset in range(ep_count)]))
    if not aligned:
        projected = jnp.take(projected, ep_place ^ jnp.arange(ep_count), axis=0)
        projected = projected.transpose(1, 0, 2).reshape(sequences, features)
    partials = [projected] + [swap(projected, "tp", offset) for offset in range(1, tp_count)]

    pick_count = expert_ids.shape[1]
    local_experts = gate_experts.shape[0]
    experts = local_experts * ep_count
    capacity = max(2, (2 * pick_count * sequences + experts - 1) // experts)
    capacity = -(-capacity // 8) * 8
    residual, outgoing = pl.pallas_call(
        functools.partial(residual_body, capacity, experts),
        out_shape=(
            made((sequences, features), bf16),
            made((experts, capacity, features), bf16),
        ),
        in_specs=[VMEM] * (4 + tp_count),
        out_specs=(VMEM, VMEM),
        name="residual",
        compiler_params=GRANT,
    )(
        *near(
            expert_ids,
            hidden,
            post_gain.reshape(1, features),
            ffn_gain.reshape(1, features),
            *partials,
        )
    )
    arrived = lax.all_to_all(outgoing, "ep", 0, 0, tiled=True)
    arrived = arrived.reshape(ep_count, local_experts, capacity, features)

    slice_width = features // tp_count
    results = []
    for own in range(local_experts):
        weights = (gate_experts[own], up_experts[own], down_experts[own])
        results.append(
            pl.pallas_call(
                expert_body,
                out_shape=made((ep_count, tp_count, capacity, slice_width), bf16),
                in_specs=[VMEM] * 2 + [HBM] * 2,
                out_specs=VMEM,
                scratch_shapes=[pltpu.VMEM(array.shape, bf16) for array in weights[1:]]
                + [pltpu.SemaphoreType.DMA((2,))],
                name="expert",
                compiler_params=GRANT,
            )(*near(arrived[:, own], weights[0]), *far(*weights[1:]))
        )
    partial_out = results[0] if local_experts == 1 else jnp.concatenate(results, axis=2)
    rows = local_experts * capacity
    flat = partial_out.reshape(ep_count * tp_count, rows, slice_width)
    returned = lax.all_to_all(flat, ("ep", "tp"), 0, 0, tiled=True)
    table = returned.reshape(ep_count, tp_count, rows, slice_width)
    combined, squares = pl.pallas_call(
        functools.partial(combine_body, capacity, experts),
        out_shape=(made((sequences, slice_width), f32), made((sequences, 128), f32)),
        in_specs=[VMEM] * 3,
        out_specs=(VMEM, VMEM),
        name="combine",
        compiler_params=GRANT,
    )(*near(expert_ids, route_logits, table))
    every = [squares] + [swap(squares, "tp", offset) for offset in range(1, tp_count)]
    return pl.pallas_call(
        functools.partial(finish_body, features),
        out_shape=jax.ShapeDtypeStruct((sequences, slice_width), bf16),
        in_specs=[SMEM] + [VMEM] * (3 + tp_count),
        out_specs=VMEM,
        name="finish",
        compiler_params=GRANT,
    )(tp_place, *near(residual, combined, out_gain.reshape(1, slice_width), *every))


def solution(mesh):
    placed = (
        P("ep", None),
        P(),
        P("ep", "tp"),
        P("ep", "tp", None),
        P("ep", "tp", None),
        P("ep"),
        P("tp"),
        P("tp", "ep"),
        P(),
        P(),
        P("ep", None),
        P("ep", None),
        P("ep", None, "tp"),
        P("ep", None, "tp"),
        P("ep", "tp", None),
        P("tp"),
    )

    return jax.shard_map(
        per_device, mesh=mesh, in_specs=placed, out_specs=P("ep", "tp"), check_vma=False
    )
```
